32 devices in a mesh: ep: 8 (over z, x), tp: 4 (over y, core).
Axes of the slice: x: 2, y: 2, z: 4, core: 2. Of those that a mesh axis runs over, the one named last changes fastest.
Arguments:
- tokens_a: bfloat16 [2048, 2048], P('ep', 'tp'), may hold values from -60 to 60
- norm_gain_a: float32 [2048], P('tp'), may hold values from 0.1 to 1.9
- pool_weight: bfloat16 [4, 512, 512], P('tp'), may hold values from -0.25 to 0.25
- pool_scale: float32 [2048], P('tp'), may hold values from 0.1 to 1.9
- tokens_b: bfloat16 [2048, 2048], P('ep'), may hold values from -6 to 6
- norm_gain_b: float32 [2048], replicated, may hold values from 0.1 to 1.9
- routes: int32 [2048, 2], P('ep'), may hold values from 0 to 7, all different within a row; in each aligned block of 256 rows (0 to 255, 256 to 511, ...) at most 96 rows name the same one
- route_logits: float32 [2048, 2], P('ep'), may hold values from -4 to 4
- expert_gate: bfloat16 [8, 2048, 3584], P('ep', None, 'tp'), may hold values from -0.125 to 0.125
- expert_up: bfloat16 [8, 2048, 3584], P('ep', None, 'tp'), may hold values from -0.125 to 0.125
- expert_down: bfloat16 [8, 3584, 2048], P('ep', 'tp'), may hold values from -0.09375 to 0.09375
Outputs:
- mixed_a: bfloat16 [2048, 2048], P('ep', 'tp')
- moe_out: bfloat16 [2048, 2048], P('ep', 'tp')
The draws below stay inside these ranges and needn't reach their ends.
Inputs may be any that keep to these rules, and one draw needn't show every extreme that they name: `routes`: among the 256 rows of one index of ep, at most 96 rows name any one expert, a bound that some block reaches.
All inputs are finite; a program needn't handle non-finite values.
Results may differ from the reference program's by a relative error of at most 0.012.
Values may be sent and summed in bfloat16 or wider, within the bound.
A program may use at most 128 MiB of HBM per device.

```python
import math
import jax
import jax.numpy as jnp
import numpy as np
from jax import lax

D = 2048
GROUPS = 4
GC = 512
FF = 3584
FF_PART = 896
TOP = 2
TOK_DEV = 256
TOKENS = 2048
EXPERTS = 8
CAP = 96
N_EP = 8
N_TP = 4


def draw_tokens_a(key, part):
    column = jnp.arange(D, dtype=jnp.float32) / D
    column_scale = jnp.exp(jnp.log(10.0) * column)
    base = jnp.clip(jax.random.normal(key, (TOKENS, D), jnp.float32), -6.0, 6.0)
    return (base * column_scale[None, :]).astype(jnp.bfloat16)


def shard_levels(own_key, dims, pieces, smallest, top_value):
    level, own = 1.0, jax.random.fold_in(own_key, 6)
    for axis_at, parts in pieces:
        steps = jnp.exp(jax.random.uniform(jax.random.fold_in(own, axis_at), (parts,), jnp.float32, smallest / len(pieces), top_value / len(pieces)))
        level = level * jnp.repeat(steps, dims[axis_at] // parts).reshape([-1 if axis == axis_at else 1 for axis in range(len(dims))])
    return level


def assign_block(stream_key, own, number, rows, amount, top, limit, skew):
    ranking = jax.random.permutation(stream_key, amount)
    packed, common = portions_of(amount, rows * top, limit, skew, True), portions_of(amount, rows * top, limit, skew, False)
    places = jnp.arange(amount)

    def named(lengths, rotation):
        used = int((lengths > 0).sum())
        fixed = max(1, used // 4)
        passed = fixed + (places - fixed + rotation * (used - fixed)) % max(1, amount - fixed)
        return jnp.zeros((amount,), jnp.int32).at[ranking[jnp.where(places < fixed, places, passed)]].set(jnp.asarray(lengths, jnp.int32))

    lengths = jnp.where(number % 4 == 0, named(packed, number // 4), named(common, number - number // 4 - 1))
    mixed = jax.random.permutation(jax.random.fold_in(own, 3), amount)
    donor, taker = mixed[0:amount // 2 * 2:2], mixed[1:amount // 2 * 2:2]
    margin = jnp.minimum(lengths[donor] - 1, limit - lengths[taker]) // 2
    margin = jnp.where((donor == ranking[0]) | (taker == ranking[0]) | (lengths[taker] == 0), 0, jnp.maximum(margin, 0))
    passed = jax.random.randint(jax.random.fold_in(own, 4), (amount // 2,), 0, 1 << 20) % (margin + 1)
    lengths = lengths.at[donor].add(-passed).at[taker].add(passed)
    members = jnp.searchsorted(jnp.cumsum(lengths), jnp.arange(rows * top), side="right").astype(jnp.int32)
    table = members.reshape(top, rows).T
    table = table[jax.random.permutation(jax.random.fold_in(own, 1), rows)]
    rotation = jax.random.randint(jax.random.fold_in(own, 2), (rows, 1), 0, top)
    return jnp.take_along_axis(table, (jnp.arange(top)[None, :] + rotation) % top, axis=1)


def portions_of(amount, total, bound, skew, full):
    loads = [(1 << 20) // math.isqrt(standing ** skew) + 1 for standing in range(1, amount + 1)]
    largest = bound if full else min(bound, max(-(-total // amount), total * loads[0] // sum(loads)))
    least = 1 if total - largest >= amount - 1 else 0
    holding, rest = [largest] + [least] * (amount - 1), total - largest - least * (amount - 1)
    while rest > 0:
        movable = [i for i in range(1, amount) if holding[i] < largest] or [i for i in range(1, amount) if holding[i] < bound]
        whole, remaining = sum([loads[i] for i in movable]), rest
        for i in movable:
            more = min(bound - holding[i], max(1, remaining * loads[i] // whole), rest)
            holding[i] = holding[i] + more
            rest = rest - more
    return np.array(holding)


def centred(stream_key, shape, width, limit, pieces=(), kind=jnp.bfloat16):
    values = jax.random.normal(stream_key, shape, jnp.float32) * width
    if len(pieces) > 0:
        values = shard_levels(stream_key, shape, pieces, -0.22, 0.18) * values
    return jnp.clip(values, min=-limit, max=limit).astype(kind)


def setup_inputs(seed: int = 0) -> dict:
    arg_keys = jax.random.split(jax.random.key(seed), 12)
    tokens_a = draw_tokens_a(jax.random.fold_in(arg_keys[11], 71), 0)
    norm_gain_a = jnp.clip(1.0 + 0.18 * jax.random.normal(arg_keys[1], (D,), jnp.float32), 0.1, 1.9)
    pool_weight = centred(arg_keys[2], (GROUPS, GC, GC), GC ** -0.5, 0.25, ((0, 4),))
    pool_scale = jnp.clip(1.0 + 0.18 * jax.random.normal(arg_keys[3], (D,), jnp.float32), 0.1, 1.9)
    tokens_b = centred(arg_keys[4], (TOKENS, D), 1.0, 6.0, ((0, 8),))
    norm_gain_b = jnp.clip(1.0 + 0.18 * jax.random.normal(arg_keys[5], (D,), jnp.float32), 0.1, 1.9)
    routes_keys = jax.random.split(jax.random.fold_in(arg_keys[6], 1), TOKENS // TOK_DEV)
    routes_turns = jax.random.permutation(jax.random.fold_in(arg_keys[6], 3), TOKENS // TOK_DEV)
    routes = jax.vmap(lambda own, number: assign_block(jax.random.fold_in(arg_keys[6], 2), own, number, TOK_DEV, EXPERTS, TOP, CAP, 1))(routes_keys, routes_turns).reshape((TOKENS, TOP))
    route_logits = centred(arg_keys[7], (TOKENS, TOP), 1.0, 4.0, ((0, 8),), jnp.float32)
    expert_gate = centred(arg_keys[8], (EXPERTS, D, FF), D ** -0.5, 0.125, ((0, 8), (2, 4)))
    expert_up = centred(arg_keys[9], (EXPERTS, D, FF), D ** -0.5, 0.125, ((0, 8), (2, 4)))
    expert_down = centred(arg_keys[10], (EXPERTS, FF, D), FF ** -0.5, 0.09375, ((0, 8), (1, 4)))
    return dict(tokens_a=tokens_a, norm_gain_a=norm_gain_a, pool_weight=pool_weight, pool_scale=pool_scale, tokens_b=tokens_b, norm_gain_b=norm_gain_b, routes=routes, route_logits=route_logits, expert_gate=expert_gate, expert_up=expert_up, expert_down=expert_down)


epsilon = 1e-06

def rms_norm(values, scale_gain):
    floats = values.astype(jnp.float32)
    scaled = floats * lax.rsqrt(lax.optimization_barrier(jnp.mean(floats * floats, axis=-1, keepdims=True)) + epsilon)
    return (scaled * scale_gain.astype(jnp.float32)).astype(jnp.bfloat16)

def reference(tokens_a, norm_gain_a, pool_weight, pool_scale, tokens_b, norm_gain_b, routes, route_logits, expert_gate, expert_up, expert_down):
    normed_a = rms_norm(tokens_a, norm_gain_a).astype(jnp.float32)
    position = jnp.arange(1, TOKENS + 1, dtype=jnp.float32)[:, None]
    outputs = []
    for group_index in range(GROUPS):
        window = 2 ** (group_index + 1)
        column = normed_a[:, group_index * GC:(group_index + 1) * GC]
        padded = jnp.pad(column, ((window - 1, 0), (0, 0)))
        pooled = jnp.zeros_like(column)
        for offset in range(window):
            begin_row = window - 1 - offset
            pooled = pooled + padded[begin_row:begin_row + TOKENS]
        pooled = pooled / jnp.minimum(position, jnp.float32(window))
        difference = (pooled - column).astype(jnp.bfloat16)
        product = jnp.dot(difference, pool_weight[group_index], preferred_element_type=jnp.float32)
        outputs.append((product * pool_scale[group_index * GC:(group_index + 1) * GC]).astype(jnp.bfloat16))
    mixed_a = jnp.concatenate(outputs, axis=1)
    normed_b = rms_norm(tokens_b, norm_gain_b)
    logit_exp = jnp.exp(route_logits)
    route_weight = logit_exp / lax.optimization_barrier(jnp.sum(logit_exp, axis=1, keepdims=True))
    flat_expert = routes.reshape(-1).astype(jnp.int32)
    onehot = (flat_expert[:, None] == jnp.arange(EXPERTS, dtype=jnp.int32)[None, :]).astype(jnp.int32)
    blocked = onehot.reshape(N_EP, TOK_DEV * TOP, EXPERTS)
    earlier = (jnp.cumsum(blocked, axis=1) - blocked).reshape(TOKENS * TOP, EXPERTS)
    position_in = lax.optimization_barrier(jnp.sum(earlier * onehot, axis=1)).astype(jnp.int32)
    source = jnp.arange(TOKENS * TOP, dtype=jnp.int32) // (TOK_DEV * TOP)
    slot_count = N_EP * CAP
    slot_index = flat_expert * slot_count + source * CAP + position_in
    token_of = jnp.arange(TOKENS * TOP, dtype=jnp.int32) // TOP
    slot_token = jnp.full((EXPERTS * slot_count,), TOKENS, jnp.int32).at[slot_index].set(token_of)
    slot_weight = jnp.zeros((EXPERTS * slot_count,), jnp.float32).at[slot_index].set(route_weight.reshape(-1))

    def expert_step(accumulated, inputs):
        gate_weight, up_weight, down_weight, chosen, weight = inputs
        row_block = jnp.take(normed_b, chosen, axis=0, mode='fill', fill_value=0)
        gate_part = jnp.dot(row_block, gate_weight, preferred_element_type=jnp.float32)
        up_part = jnp.dot(row_block, up_weight, preferred_element_type=jnp.float32)
        hidden = (jax.nn.silu(gate_part) * up_part).astype(jnp.bfloat16)
        result = jnp.zeros((slot_count, D), jnp.float32)
        for part_index in range(N_TP):
            lower = part_index * FF_PART
            piece = jnp.dot(hidden[:, lower:lower + FF_PART], down_weight[lower:lower + FF_PART], preferred_element_type=jnp.float32)
            rounded = lax.optimization_barrier(piece.astype(jnp.bfloat16))
            result = result + rounded.astype(jnp.float32)
        accumulated = accumulated.at[chosen].add(result * weight[:, None], mode='drop')
        return (accumulated, None)
    accumulated, _ = lax.scan(expert_step, jnp.zeros((TOKENS, D), jnp.float32), (expert_gate, expert_up, expert_down, slot_token.reshape(EXPERTS, slot_count), slot_weight.reshape(EXPERTS, slot_count)))
    moe_out = accumulated.astype(jnp.bfloat16)
    return (mixed_a, moe_out)
```

```python
import functools

import jax
import jax.numpy as jnp
from jax import lax
from jax.experimental import pallas as pl
from jax.experimental.pallas import tpu as pltpu
from jax.sharding import PartitionSpec as P

GROUPS = 4
TOP = 2
MESH = pl.DeviceIdType.MESH
F32 = jnp.float32
BF16 = jnp.bfloat16

epsilon = 1e-06


def dot(a, b):
    return jnp.dot(a, b, preferred_element_type=F32)


def body(
    n,
    cap,
    group,
    ta_ref,
    ga_ref,
    pw_ref,
    ps_ref,
    tb_ref,
    gb_ref,
    rt_ref,
    rc_ref,
    rl_ref,
    wg_hbm,
    wu_hbm,
    wd_hbm,
    mixed_ref,
    moe_ref,
    wg,
    wu,
    wd,
    nb,
    outgoing,
    rows,
    part,
    core_in,
    y_out,
    y_in,
    back_out,
    back_in,
    sq,
    rim_out,
    rim_in,
    w_sem,
    send,
    recv,
    sq_send,
    sq_recv,
    rim_send,
    rim_recv,
):
    ep = lax.axis_index("ep")
    tp = lax.axis_index("tp")
    core = lax.rem(tp, 2)
    y = lax.div(tp, 2)
    core_peer = tp + 1 - 2 * core
    y_peer = lax.rem(tp + 2, 4)
    cross_peer = lax.rem(core_peer + 2, 4)
    tok, quarter = ta_ref.shape
    groups = n // group

    barrier = pltpu.get_barrier_semaphore()

    def greet(k, _):
        pl.semaphore_signal(
            barrier,
            inc=1,
            device_id={"ep": lax.rem(ep + k, n), "tp": tp},
            device_id_type=MESH,
        )
        return 0

    lax.fori_loop(1, n, greet, 0)
    for peer in (core_peer, y_peer, cross_peer):
        pl.semaphore_signal(
            barrier, inc=1, device_id={"ep": ep, "tp": peer}, device_id_type=MESH
        )
    weights = [
        pltpu.make_async_copy(src.at[0], dst, w_sem.at[i])
        for i, (src, dst) in enumerate(((wg_hbm, wg), (wu_hbm, wu), (wd_hbm, wd)))
    ]
    for copy in weights:
        copy.start()

    def offset_of(j):
        half = lax.div(j + 1, 2)
        return jnp.where(lax.rem(j, 2) == 1, half, lax.rem(n - half, n))

    def remote(kind, j, src, dst, peer_ep, peer_tp):
        return pltpu.make_async_remote_copy(
            src_ref=src,
            dst_ref=dst,
            send_sem=send.at[kind, j],
            recv_sem=recv.at[kind, j],
            device_id={"ep": peer_ep, "tp": peer_tp},
            device_id_type=MESH,
        )

    def columns(index):
        return pl.ds(pl.multiple_of(index * quarter, quarter), quarter)

    def dispatch(j):
        return remote(
            0,
            j,
            outgoing.at[j],
            rows.at[j, :, columns(tp)],
            lax.rem(ep + offset_of(j), n),
            tp,
        )

    def to_core(j):
        view = rows.at[j, :, columns(tp)]
        return remote(1, j, view, view, ep, core_peer)

    def to_y(j):
        view = rows.at[j, :, columns(tp)]
        return remote(2, j, view, view, ep, y_peer)

    def relay(j):
        view = rows.at[j, :, columns(y_peer)]
        return remote(3, j, view, view, ep, core_peer)

    def part_core(j):
        return remote(4, j, part.at[1 - core, j], core_in.at[j], ep, core_peer)

    def part_y(j):
        return remote(5, j, y_out.at[j], y_in.at[j], ep, y_peer)

    def give_back(j):
        return remote(
            6,
            j,
            back_out.at[j],
            back_in.at[j],
            lax.rem(ep - offset_of(j) + n, n),
            tp,
        )

    rows_a = ta_ref[...].astype(F32)
    own_sq = jnp.sum(rows_a * rows_a, axis=1, keepdims=True)
    sq[0] = jnp.transpose(jnp.broadcast_to(own_sq, (tok, 128)))[:8]

    floats_b = tb_ref[...].astype(F32)
    scale_b = lax.rsqrt(
        jnp.mean(floats_b * floats_b, axis=1, keepdims=True) + epsilon
    )
    nb[...] = (floats_b * scale_b * gb_ref[...]).astype(BF16)

    def slot_of(expert, place):
        k = expert - ep
        k = jnp.where(k < 0, k + n, k)
        j = jnp.where(k == 0, 0, jnp.where(2 * k <= n, 2 * k - 1, 2 * (n - k)))
        return j * cap + place

    def slots(axis):
        shape = (n, tok) if axis == 0 else (tok, n)
        ref = rt_ref if axis == 0 else rc_ref
        experts = [
            ref[k : k + 1, :] if axis == 0 else ref[:, k : k + 1] for k in range(TOP)
        ]
        index = lax.broadcasted_iota(jnp.int32, shape, axis)
        hot = [(index == e).astype(F32) for e in experts]
        before = (
            lax.broadcasted_iota(jnp.int32, (tok, tok), axis)
            < lax.broadcasted_iota(jnp.int32, (tok, tok), 1 - axis)
        ).astype(F32).astype(BF16)
        total = (hot[0] + hot[1]).astype(BF16)
        earlier = dot(total, before) if axis == 0 else dot(before, total)
        return [
            slot_of(
                e, jnp.sum(earlier * h, axis=axis, keepdims=True).astype(jnp.int32)
            )
            for e, h in zip(experts, hot)
        ]

    lane_slots = slots(0)
    chosen = lax.broadcasted_iota(jnp.int32, (n * cap, tok), 0)
    hot = (
        ((chosen == lane_slots[0]) | (chosen == lane_slots[1]))
        .astype(F32)
        .astype(BF16)
    )
    outgoing[...] = (
        dot(hot, nb[:, columns(tp)]).astype(BF16).reshape(n, cap, quarter)
    )

    pl.semaphore_wait(barrier, n + 2)
    sq_copies = [
        pltpu.make_async_remote_copy(
            src_ref=sq.at[0],
            dst_ref=sq.at[i],
            send_sem=sq_send.at[i - 1],
            recv_sem=sq_recv.at[i - 1],
            device_id={"ep": ep, "tp": peer},
            device_id_type=MESH,
        )
        for i, peer in ((1, core_peer), (2, y_peer), (3, cross_peer))
    ]
    for copy in sq_copies:
        copy.start()

    def start_dispatch(j, _):
        dispatch(j).start()
        return 0

    lax.fori_loop(1, n, start_dispatch, 0)
    rows[0] = dot(hot[:cap], nb[...]).astype(BF16)

    for copy in sq_copies:
        copy.wait_recv()
    total_sq = (sq[0] + sq[1]) + (sq[2] + sq[3])
    squares = jnp.transpose(jnp.broadcast_to(total_sq[:1], (128, tok)))[:, :1]
    width = quarter * 4
    normed_a = (rows_a * lax.rsqrt(squares / width + epsilon) * ga_ref[...]).astype(
        BF16
    )
    widest = 2**GROUPS
    rim_out[...] = normed_a[tok - widest :]
    rim = pltpu.make_async_remote_copy(
        src_ref=rim_out,
        dst_ref=rim_in,
        send_sem=rim_send,
        recv_sem=rim_recv,
        device_id={"ep": lax.rem(ep + 1, n), "tp": tp},
        device_id_type=MESH,
    )
    rim.start()

    def forward(g):
        def step(j, _):
            @pl.when(j > 0)
            def _():
                dispatch(j).wait_recv()
                to_core(j).start()
                to_y(j).start()

            return 0

        lax.fori_loop(g * group, (g + 1) * group, step, 0)

    forward(0)

    rim.wait_recv()
    before_own = jnp.where(ep == 0, 0.0, rim_in[...].astype(F32))
    own = normed_a.astype(F32)
    pooled = jnp.concatenate([before_own, own], axis=0)
    wanted = None
    for level in range(GROUPS):
        pooled = pooled + pltpu.roll(pooled, 2**level, 0)
        wanted = pooled if wanted is None else jnp.where(tp >= level, pooled, wanted)
    window_len = jnp.left_shift(jnp.int32(1), tp + 1)
    position = ep * tok + 1 + lax.broadcasted_iota(jnp.int32, (tok, 1), 0)
    divisor = jnp.minimum(position, window_len).astype(F32)
    difference = (wanted[widest:] / divisor - own).astype(BF16)
    mixed_ref[...] = (dot(difference, pw_ref[0]) * ps_ref[...]).astype(BF16)

    for copy in weights:
        copy.wait()

    def sum_y(j, _):
        part_core(j).wait_recv()
        away = columns(1 - y)
        y_out[j] = (
            part[core, j, :, away].astype(F32) + core_in[j, :, away].astype(F32)
        ).astype(BF16)
        part_y(j).start()
        return 0

    def sum_all(j, _):
        part_y(j).wait_recv()
        here = columns(y)
        value = (
            part[core, j, :, here].astype(F32)
            + core_in[j, :, here].astype(F32)
            + y_in[j].astype(F32)
        ).astype(BF16)

        @pl.when(j > 0)
        def _():
            back_out[j] = value
            give_back(j).start()

        @pl.when(j == 0)
        def _():
            back_in[j] = value

        return 0

    def compute(g, _):
        first, last = g * group, (g + 1) * group

        def pass_on(j, _):
            @pl.when(j > 0)
            def _():
                to_y(j).wait_recv()
                relay(j).start()

            return 0

        def arrived(j, _):
            @pl.when(j > 0)
            def _():
                to_core(j).wait_recv()
                relay(j).wait_recv()

            return 0

        lax.fori_loop(first, last, pass_on, 0)
        lax.fori_loop(first, last, arrived, 0)
        block = rows[pl.ds(first, group)].reshape(group * cap, width)
        gate = dot(block, wg[...])
        up = dot(block, wu[...])
        hidden = (gate / (1.0 + jnp.exp(-gate)) * up).astype(BF16)
        for q in range(4):
            piece = dot(hidden, wd[:, q * quarter : (q + 1) * quarter]).astype(BF16)
            half = (q // 2) * quarter
            part[q % 2, pl.ds(first, group), :, half : half + quarter] = piece.reshape(
                group, cap, quarter
            )

        def start_part(j, _):
            part_core(j).start()
            return 0

        lax.fori_loop(first, last, start_part, 0)

        @pl.when(g + 1 < groups)
        def _():
            forward(g + 1)

        lax.fori_loop(first, last, sum_y, 0)

        @pl.when(g > 0)
        def _():
            lax.fori_loop(first - group, last - group, sum_all, 0)

        return 0

    lax.fori_loop(0, groups, compute, 0)
    lax.fori_loop(n - group, n, sum_all, 0)

    def finish(j, _):
        part_core(j).wait_send()
        part_y(j).wait_send()

        @pl.when(j > 0)
        def _():
            dispatch(j).wait_send()
            to_core(j).wait_send()
            to_y(j).wait_send()
            relay(j).wait_send()
            give_back(j).wait_send()
            give_back(j).wait_recv()

        return 0

    weight_exp = jnp.exp(rl_ref[...])
    route_weight = weight_exp / jnp.sum(weight_exp, axis=1, keepdims=True)
    chosen = lax.broadcasted_iota(jnp.int32, (tok, n * cap), 1)
    picks = [(chosen == s).astype(F32).astype(BF16) for s in slots(1)]
    for copy in sq_copies:
        copy.wait_send()
    rim.wait_send()
    lax.fori_loop(0, n, finish, 0)
    flat = back_in[...].reshape(n * cap, quarter)
    combined = jnp.zeros((tok, quarter), F32)
    for k in range(TOP):
        combined = combined + dot(picks[k], flat) * route_weight[:, k : k + 1]
    moe_ref[...] = combined.astype(BF16)


def shards(
    n,
    tokens_a,
    norm_gain_a,
    pool_weight,
    pool_scale,
    tokens_b,
    norm_gain_b,
    routes,
    route_logits,
    expert_gate,
    expert_up,
    expert_down,
):
    tok, width = tokens_b.shape
    quarter = tokens_a.shape[1]
    hidden = expert_gate.shape[2]
    most = max(2, (3 * TOP * tok + 2 * n - 1) // (2 * n))
    cap = -(-most // 16) * 16
    group = 1
    while n % (2 * group) == 0 and 2 * group * cap <= 256:
        group = 2 * group
    vmem = pl.BlockSpec(memory_space=pltpu.VMEM)
    hbm = pl.BlockSpec(memory_space=pl.ANY)
    slab = pltpu.VMEM((n, cap, quarter), BF16)
    dma = pltpu.SemaphoreType.DMA
    return pl.pallas_call(
        functools.partial(body, n, cap, group),
        out_shape=(
            jax.ShapeDtypeStruct((tok, quarter), BF16),
            jax.ShapeDtypeStruct((tok, quarter), BF16),
        ),
        in_specs=[vmem] * 9 + [hbm] * 3,
        out_specs=(vmem, vmem),
        scratch_shapes=[
            pltpu.VMEM((width, hidden), BF16),
            pltpu.VMEM((width, hidden), BF16),
            pltpu.VMEM((hidden, width), BF16),
            pltpu.VMEM((tok, width), BF16),
            slab,
            pltpu.VMEM((n, cap, width), BF16),
            pltpu.VMEM((2, n, cap, 2 * quarter), BF16),
            pltpu.VMEM((n, cap, 2 * quarter), BF16),
            slab,
            slab,
            slab,
            slab,
            pltpu.VMEM((4, 8, tok), F32),
            pltpu.VMEM((2**GROUPS, quarter), BF16),
            pltpu.VMEM((2**GROUPS, quarter), BF16),
            dma((3,)),
            dma((7, n)),
            dma((7, n)),
            dma((3,)),
            dma((3,)),
            dma,
            dma,
        ],
        compiler_params=pltpu.CompilerParams(
            collective_id=0,
            has_side_effects=True,
            vmem_limit_bytes=60 * 1024 * 1024,
        ),
    )(
        tokens_a,
        norm_gain_a[None, :],
        pool_weight,
        pool_scale[None, :],
        tokens_b,
        norm_gain_b[None, :],
        routes.T,
        routes,
        route_logits,
        expert_gate,
        expert_up,
        expert_down,
    )


def solution(mesh):
    placed = (
        P("ep", "tp"),
        P("tp"),
        P("tp", None, None),
        P("tp"),
        P("ep", None),
        P(),
        P("ep", None),
        P("ep", None),
        P("ep", None, "tp"),
        P("ep", None, "tp"),
        P("ep", "tp", None),
    )
    return jax.shard_map(
        functools.partial(shards, mesh.shape["ep"]),
        mesh=mesh,
        in_specs=placed,
        out_specs=(P("ep", "tp"), P("ep", "tp")),
        check_vma=False,
    )
```

```python
import functools

import jax
import jax.numpy as jnp
from jax import lax
from jax.experimental import pallas as pl
from jax.experimental.pallas import tpu as pltpu
from jax.sharding import PartitionSpec as P

GROUPS = 4
TOP = 2
MESH = pl.DeviceIdType.MESH
F32 = jnp.float32
BF16 = jnp.bfloat16

epsilon = 1e-06


def dot(a, b):
    return jnp.dot(a, b, preferred_element_type=F32)


def body(
    n,
    cap,
    group,
    ta_ref,
    ga_ref,
    pw_ref,
    ps_ref,
    tb_ref,
    gb_ref,
    rt_ref,
    rl_ref,
    wg_hbm,
    wu_hbm,
    wd_hbm,
    both_ref,
    wg,
    wu,
    wd,
    nb,
    outgoing,
    rows,
    part,
    core_in,
    y_out,
    y_in,
    back_out,
    back_in,
    sq,
    rim_out,
    rim_in,
    w_sem,
    send,
    recv,
    sq_send,
    sq_recv,
    rim_send,
    rim_recv,
):
    ep = lax.axis_index("ep")
    tp = lax.axis_index("tp")
    core = lax.rem(tp, 2)
    y = lax.div(tp, 2)
    core_peer = tp + 1 - 2 * core
    y_peer = lax.rem(tp + 2, 4)
    cross_peer = lax.rem(core_peer + 2, 4)
    tok, quarter = ta_ref.shape
    groups = n // group

    barrier = pltpu.get_barrier_semaphore()

    def greet(k, _):
        pl.semaphore_signal(
            barrier,
            inc=1,
            device_id={"ep": lax.rem(ep + k, n), "tp": tp},
            device_id_type=MESH,
        )
        return 0

    lax.fori_loop(1, n, greet, 0)
    for peer in (core_peer, y_peer, cross_peer):
        pl.semaphore_signal(
            barrier, inc=1, device_id={"ep": ep, "tp": peer}, device_id_type=MESH
        )
    weights = [
        pltpu.make_async_copy(src.at[0], dst, w_sem.at[i])
        for i, (src, dst) in enumerate(((wg_hbm, wg), (wu_hbm, wu), (wd_hbm, wd)))
    ]
    for copy in weights:
        copy.start()

    def offset_of(j):
        half = lax.div(j + 1, 2)
        return jnp.where(lax.rem(j, 2) == 1, half, lax.rem(n - half, n))

    def remote(kind, j, src, dst, peer_ep, peer_tp):
        return pltpu.make_async_remote_copy(
            src_ref=src,
            dst_ref=dst,
            send_sem=send.at[kind, j],
            recv_sem=recv.at[kind, j],
            device_id={"ep": peer_ep, "tp": peer_tp},
            device_id_type=MESH,
        )

    def columns(index):
        return pl.ds(pl.multiple_of(index * quarter, quarter), quarter)

    def dispatch(j):
        return remote(
            0,
            j,
            outgoing.at[j],
            rows.at[j, :, columns(tp)],
            lax.rem(ep + offset_of(j), n),
            tp,
        )

    def span(g):
        if isinstance(g, int) and g == 0:
            return pl.ds(1, group - 1)
        return pl.ds(g * group, group)

    def to_core(g):
        view = rows.at[span(g), :, columns(tp)]
        return remote(1, g, view, view, ep, core_peer)

    def to_y(g):
        view = rows.at[span(g), :, columns(tp)]
        return remote(2, g, view, view, ep, y_peer)

    def relay(g):
        view = rows.at[span(g), :, columns(y_peer)]
        return remote(3, g, view, view, ep, core_peer)

    def part_core(g):
        many = pl.ds(g * group, group)
        return remote(
            4, g, part.at[1 - core, many], core_in.at[many], ep, core_peer
        )

    def part_y(g):
        many = pl.ds(g * group, group)
        return remote(5, g, y_out.at[many], y_in.at[many], ep, y_peer)

    def each(g, act):
        if isinstance(g, int):
            if g > 0 or group > 1:
                act(g)
            return
        if group > 1:

            @pl.when(g == 0)
            def _():
                act(0)

        @pl.when(g > 0)
        def _():
            act(g)

    def give_back(j):
        return remote(
            6,
            j,
            back_out.at[j],
            back_in.at[j],
            lax.rem(ep - offset_of(j) + n, n),
            tp,
        )

    rows_a = ta_ref[...].astype(F32)
    own_sq = jnp.sum(rows_a * rows_a, axis=1, keepdims=True)
    sq[0] = jnp.transpose(jnp.broadcast_to(own_sq, (tok, 128)))[:8]

    floats_b = tb_ref[...].astype(F32)
    scale_b = lax.rsqrt(
        jnp.mean(floats_b * floats_b, axis=1, keepdims=True) + epsilon
    )
    nb[...] = (floats_b * scale_b * gb_ref[...]).astype(BF16)

    def slot_of(expert, place):
        k = expert - ep
        k = jnp.where(k < 0, k + n, k)
        j = jnp.where(k == 0, 0, jnp.where(2 * k <= n, 2 * k - 1, 2 * (n - k)))
        return j * cap + place

    experts = [rt_ref[k : k + 1, :] for k in range(TOP)]
    index = lax.broadcasted_iota(jnp.int32, (n, tok), 0)
    named = [(index == e).astype(F32) for e in experts]
    before = (
        (
            lax.broadcasted_iota(jnp.int32, (tok, tok), 0)
            < lax.broadcasted_iota(jnp.int32, (tok, tok), 1)
        )
        .astype(F32)
        .astype(BF16)
    )
    earlier = dot((named[0] + named[1]).astype(BF16), before)
    lane_slots = [
        slot_of(e, jnp.sum(earlier * h, axis=0, keepdims=True).astype(jnp.int32))
        for e, h in zip(experts, named)
    ]
    chosen = lax.broadcasted_iota(jnp.int32, (n * cap, tok), 0)
    hot = (
        ((chosen == lane_slots[0]) | (chosen == lane_slots[1]))
        .astype(F32)
        .astype(BF16)
    )
    outgoing[...] = (
        dot(hot, nb[:, columns(tp)]).astype(BF16).reshape(n, cap, quarter)
    )

    pl.semaphore_wait(barrier, n + 2)
    sq_copies = [
        pltpu.make_async_remote_copy(
            src_ref=sq.at[0],
            dst_ref=sq.at[i],
            send_sem=sq_send.at[i - 1],
            recv_sem=sq_recv.at[i - 1],
            device_id={"ep": ep, "tp": peer},
            device_id_type=MESH,
        )
        for i, peer in ((1, core_peer), (2, y_peer), (3, cross_peer))
    ]
    for copy in sq_copies:
        copy.start()

    def start_dispatch(j, _):
        dispatch(j).start()
        return 0

    lax.fori_loop(1, n, start_dispatch, 0)
    rows[0] = dot(hot[:cap], nb[...]).astype(BF16)

    for copy in sq_copies:
        copy.wait_recv()
    total_sq = (sq[0] + sq[1]) + (sq[2] + sq[3])
    squares = jnp.transpose(jnp.broadcast_to(total_sq[:1], (128, tok)))[:, :1]
    width = quarter * 4
    normed_a = (rows_a * lax.rsqrt(squares / width + epsilon) * ga_ref[...]).astype(
        BF16
    )
    widest = 2**GROUPS
    rim_out[...] = normed_a[tok - widest :]
    rim = pltpu.make_async_remote_copy(
        src_ref=rim_out,
        dst_ref=rim_in,
        send_sem=rim_send,
        recv_sem=rim_recv,
        device_id={"ep": lax.rem(ep + 1, n), "tp": tp},
        device_id_type=MESH,
    )
    rim.start()

    def forward(g):
        def step(j, _):
            @pl.when(j > 0)
            def _():
                dispatch(j).wait_recv()

            return 0

        lax.fori_loop(g * group, (g + 1) * group, step, 0)

        def act(g):
            to_y(g).start()
            to_core(g).start()

        each(g, act)

    forward(0)

    rim.wait_recv()
    before_own = jnp.where(ep == 0, 0.0, rim_in[...].astype(F32))
    own = normed_a.astype(F32)
    pooled = jnp.concatenate([before_own, own], axis=0)
    wanted = None
    for level in range(GROUPS):
        pooled = pooled + pltpu.roll(pooled, 2**level, 0)
        wanted = pooled if wanted is None else jnp.where(tp >= level, pooled, wanted)
    window_len = jnp.left_shift(jnp.int32(1), tp + 1)
    position = ep * tok + 1 + lax.broadcasted_iota(jnp.int32, (tok, 1), 0)
    divisor = jnp.minimum(position, window_len).astype(F32)
    difference = (wanted[widest:] / divisor - own).astype(BF16)
    both_ref[0] = dot(difference, pw_ref[0]) * ps_ref[...]

    for copy in weights:
        copy.wait()

    def sum_y(g):
        part_core(g).wait_recv()
        away, many = columns(1 - y), pl.ds(g * group, group)
        y_out[many] = (
            part[core, many, :, away].astype(F32) + core_in[many, :, away].astype(F32)
        ).astype(BF16)
        part_y(g).start()

    def sum_all(g):
        part_y(g).wait_recv()
        here = columns(y)

        def step(j, _):
            value = (
                part[core, j, :, here].astype(F32)
                + core_in[j, :, here].astype(F32)
                + y_in[j].astype(F32)
            ).astype(BF16)

            @pl.when(j > 0)
            def _():
                back_out[j] = value
                give_back(j).start()

            @pl.when(j == 0)
            def _():
                back_in[j] = value

            return 0

        lax.fori_loop(g * group, (g + 1) * group, step, 0)

    def compute(g, _):
        first = g * group

        def pass_on(g):
            to_y(g).wait_recv()
            relay(g).start()

        def arrived(g):
            to_core(g).wait_recv()
            relay(g).wait_recv()

        each(g, pass_on)
        each(g, arrived)
        block = rows[pl.ds(first, group)].reshape(group * cap, width)
        gate = dot(block, wg[...])
        up = dot(block, wu[...])
        hidden = (gate / (1.0 + jnp.exp(-gate)) * up).astype(BF16)
        for q in range(4):
            piece = dot(hidden, wd[:, q * quarter : (q + 1) * quarter]).astype(BF16)
            half = (q // 2) * quarter
            part[q % 2, pl.ds(first, group), :, half : half + quarter] = piece.reshape(
                group, cap, quarter
            )

        part_core(g).start()

        @pl.when(g + 2 < groups)
        def _():
            forward(g + 2)

        sum_y(g)

        @pl.when(g > 1)
        def _():
            sum_all(g - 2)

        return 0

    if groups > 1:
        forward(1)
    lax.fori_loop(0, groups, compute, 0)
    for g in range(max(0, groups - 2), groups):
        sum_all(g)

    def finish(j, _):
        @pl.when(j > 0)
        def _():
            dispatch(j).wait_send()
            give_back(j).wait_send()
            give_back(j).wait_recv()

        return 0

    def sent(g, _):
        part_core(g).wait_send()
        part_y(g).wait_send()

        def act(g):
            to_core(g).wait_send()
            to_y(g).wait_send()
            relay(g).wait_send()

        each(g, act)
        return 0

    weight_exp = jnp.exp(rl_ref[...])
    route_weight = weight_exp / jnp.sum(weight_exp, axis=0, keepdims=True)
    line = lax.broadcasted_iota(jnp.int32, (128, tok), 0)
    stacked = jnp.zeros((128, tok), F32)
    for i, row in enumerate(
        [s.astype(F32) for s in lane_slots]
        + [route_weight[k : k + 1, :] for k in range(TOP)]
    ):
        stacked = jnp.where(line == i, row, stacked)
    turned = jnp.transpose(stacked)
    chosen = lax.broadcasted_iota(jnp.int32, (tok, n * cap), 1)
    picks = [
        (chosen == turned[:, k : k + 1].astype(jnp.int32)).astype(F32).astype(BF16)
        for k in range(TOP)
    ]
    for copy in sq_copies:
        copy.wait_send()
    rim.wait_send()
    lax.fori_loop(0, groups, sent, 0)
    lax.fori_loop(0, n, finish, 0)
    flat = back_in[...].reshape(n * cap, quarter)
    combined = jnp.zeros((tok, quarter), F32)
    for k in range(TOP):
        combined = combined + dot(picks[k], flat) * turned[:, TOP + k : TOP + k + 1]
    both_ref[1] = combined


def shards(
    n,
    tokens_a,
    norm_gain_a,
    pool_weight,
    pool_scale,
    tokens_b,
    norm_gain_b,
    routes,
    route_logits,
    expert_gate,
    expert_up,
    expert_down,
):
    tok, width = tokens_b.shape
    quarter = tokens_a.shape[1]
    hidden = expert_gate.shape[2]
    most = max(2, (3 * TOP * tok + 2 * n - 1) // (2 * n))
    cap = -(-most // 16) * 16
    group = 1
    while n % (2 * group) == 0 and 2 * group * cap <= 256:
        group = 2 * group
    vmem = pl.BlockSpec(memory_space=pltpu.VMEM)
    hbm = pl.BlockSpec(memory_space=pl.ANY)
    slab = pltpu.VMEM((n, cap, quarter), BF16)
    dma = pltpu.SemaphoreType.DMA
    both = pl.pallas_call(
        functools.partial(body, n, cap, group),
        out_shape=jax.ShapeDtypeStruct((2, tok, quarter), F32),
        in_specs=[vmem] * 8 + [hbm] * 3,
        out_specs=vmem,
        scratch_shapes=[
            pltpu.VMEM((width, hidden), BF16),
            pltpu.VMEM((width, hidden), BF16),
            pltpu.VMEM((hidden, width), BF16),
            pltpu.VMEM((tok, width), BF16),
            slab,
            pltpu.VMEM((n, cap, width), BF16),
            pltpu.VMEM((2, n, cap, 2 * quarter), BF16),
            pltpu.VMEM((n, cap, 2 * quarter), BF16),
            slab,
            slab,
            slab,
            slab,
            pltpu.VMEM((4, 8, tok), F32),
            pltpu.VMEM((2**GROUPS, quarter), BF16),
            pltpu.VMEM((2**GROUPS, quarter), BF16),
            dma((3,)),
            dma((7, n)),
            dma((7, n)),
            dma((3,)),
            dma((3,)),
            dma,
            dma,
        ],
        compiler_params=pltpu.CompilerParams(
            collective_id=0,
            has_side_effects=True,
            vmem_limit_bytes=60 * 1024 * 1024,
        ),
    )(
        tokens_a,
        norm_gain_a[None, :],
        pool_weight,
        pool_scale[None, :],
        tokens_b,
        norm_gain_b[None, :],
        routes.T,
        route_logits.T,
        expert_gate,
        expert_up,
        expert_down,
    )
    return both[0].astype(BF16), both[1].astype(BF16)


def solution(mesh):
    placed = (
        P("ep", "tp"),
        P("tp"),
        P("tp", None, None),
        P("tp"),
        P("ep", None),
        P(),
        P("ep", None),
        P("ep", None),
        P("ep", None, "tp"),
        P("ep", None, "tp"),
        P("ep", "tp", None),
    )
    return jax.shard_map(
        functools.partial(shards, mesh.shape["ep"]),
        mesh=mesh,
        in_specs=placed,
        out_specs=(P("ep", "tp"), P("ep", "tp")),
        check_vma=False,
    )
```
